128 devices in a mesh: fs: 32 (over z, y, core), tp: 4 (over x).
Axes of the slice: x: 4, y: 4, z: 4, core: 2. Of those that a mesh axis runs over, the one named last changes fastest.
Arguments:
- hidden_states: bfloat16 [2048, 2048], P('tp', 'fs'), may hold values from -6 to 6
- norm_gain: float32 [2048], P('fs'), may hold values from 0.1 to 1.9
- gate_master: float32 [8, 2048, 7168], P(None, 'fs', 'tp'), may hold values from -0.125 to 0.125
- up_master: float32 [8, 2048, 7168], P(None, 'fs', 'tp'), may hold values from -0.125 to 0.125
- down_master: float32 [8, 2048, 7168], P(None, 'fs', 'tp'), may hold values from -0.0625 to 0.0625
- expert_ids: int32 [2048, 2], P('tp'), may hold values from 0 to 7, all different within a row; in each aligned block of 512 rows (0 to 511, 512 to 1023, ...) at most 256 rows name the same one
- route_logits: float32 [2048, 2], P('tp'), may hold values from -6 to 6
Outputs:
- gate_serve: bfloat16 [8, 2048, 7168], P('tp', None, 'fs')
- up_serve: bfloat16 [8, 2048, 7168], P('tp', None, 'fs')
- down_serve: bfloat16 [8, 2048, 7168], P('tp', None, 'fs')
- combined: bfloat16 [2048, 2048], P('tp', 'fs')
The draws below stay inside these ranges and needn't reach their ends.
Inputs may be any that keep to these rules, and one draw needn't show every extreme that they name: `expert_ids`: the 2 entries of a row differ. Among the rows of one index of tp (aligned blocks of 512 rows) no expert is named more than 256 times, and in some blocks one expert is named exactly 256 times.
All inputs are finite; a program needn't handle non-finite values.
Results may differ from the reference program's by a relative error of at most 0.018.
Values may be sent and summed in bfloat16 or wider, within the bound.
No kernel may reach another device: no remote copies, remote signals or barrier semaphores. Data moves between devices by JAX's collectives and lax.ppermute only.
A program may use at most 128 MiB of HBM per device.

```python
import math
import jax
import jax.numpy as jnp
import numpy as np
from jax import lax

D = 2048
FF = 7168
EXPERTS = 8
TOP = 2
TOK_DEV = 512
CAP = 256
TOKENS = 2048


def levels(key, dims, shards, smallest, largest):
    def one(axis_at, blocks):
        steps = jax.random.uniform(jax.random.fold_in(jax.random.fold_in(key, 6), axis_at), (blocks,), jnp.float32, smallest / len(shards), largest / len(shards))
        return jnp.repeat(jnp.exp(steps), dims[axis_at] // blocks).reshape((-1,) + (1,) * (len(dims) - axis_at - 1))

    loudness = one(*shards[0])
    for cut in shards[1:]:
        loudness = loudness * one(*cut)
    return loudness


def shared_out(key, own, number, rows, amount, top, bound, slope):
    sequence = jax.random.permutation(key, amount)
    heavy_load, ordinary = load_shares(amount, rows * top, bound, slope, True), load_shares(amount, rows * top, bound, slope, False)
    places = jnp.arange(amount)

    def named(lengths, offset_by):
        used = int((lengths > 0).sum())
        fixed = max(1, used // 4)
        passed = fixed + (places - fixed + offset_by * (used - fixed)) % max(1, amount - fixed)
        return jnp.zeros((amount,), jnp.int32).at[sequence[jnp.where(places < fixed, places, passed)]].set(jnp.asarray(lengths, jnp.int32))

    lengths = jnp.where(number % 4 == 0, named(heavy_load, number // 4), named(ordinary, number - number // 4 - 1))
    mixed = jax.random.permutation(jax.random.fold_in(own, 3), amount)
    donor, taker = mixed[0:amount // 2 * 2:2], mixed[1:amount // 2 * 2:2]
    room = jnp.minimum(lengths[donor] - 1, bound - lengths[taker]) // 2
    room = jnp.where((donor == sequence[0]) | (taker == sequence[0]) | (lengths[taker] == 0), 0, jnp.maximum(room, 0))
    passed = jax.random.randint(jax.random.fold_in(own, 4), (amount // 2,), 0, 1 << 20) % (room + 1)
    lengths = lengths.at[donor].add(-passed).at[taker].add(passed)
    labels = jnp.searchsorted(jnp.cumsum(lengths), jnp.arange(rows * top), side="right").astype(jnp.int32)
    listing = labels.reshape(top, rows).T
    listing = listing[jax.random.permutation(jax.random.fold_in(own, 1), rows)]
    offset_by = jax.random.randint(jax.random.fold_in(own, 2), (rows, 1), 0, top)
    return jnp.take_along_axis(listing, (jnp.arange(top)[None, :] + offset_by) % top, axis=1)


def load_shares(amount, total, limit, lean, full):
    loads = [(1 << 20) // math.isqrt(rank ** lean) + 1 for rank in range(1, amount + 1)]
    largest = limit if full else min(limit, max(-(-total // amount), total * loads[0] // sum(loads)))
    least = 1 if total - largest >= amount - 1 else 0
    counts, spare = [largest] + [least] * (amount - 1), total - largest - least * (amount - 1)
    while spare > 0:
        candidates = [i for i in range(1, amount) if counts[i] < largest] or [i for i in range(1, amount) if counts[i] < limit]
        whole, left = sum([loads[i] for i in candidates]), spare
        for i in candidates:
            extra = min(limit - counts[i], max(1, left * loads[i] // whole), spare)
            counts[i] = counts[i] + extra
            spare = spare - extra
    return np.array(counts)


def scatter_about(key, extent, deviation, limit, shards=(), kind=jnp.bfloat16):
    array = deviation * jax.random.normal(key, extent, jnp.float32)
    if shards:
        array = array * levels(key, extent, shards, -0.22, 0.18)
    return jnp.clip(array, -limit, limit).astype(kind)


def setup_inputs(seed: int = 0) -> dict:
    keys = jax.random.split(jax.random.key(seed), 8)
    hidden_states = scatter_about(keys[0], (TOKENS, D), 1.0, 6.0, ((0, 4), (1, 32)))
    norm_gain = jnp.clip(1.0 + 0.18 * jax.random.normal(keys[1], (D,), jnp.float32), 0.1, 1.9)
    gate_master = scatter_about(keys[2], (EXPERTS, D, FF), D ** -0.5, 0.125, ((1, 32), (2, 4)), jnp.float32)
    up_master = scatter_about(keys[3], (EXPERTS, D, FF), D ** -0.5, 0.125, ((1, 32), (2, 4)), jnp.float32)
    down_master = scatter_about(keys[4], (EXPERTS, D, FF), FF ** -0.5, 0.0625, ((1, 32), (2, 4)), jnp.float32)
    expert_ids_keys = jax.random.split(jax.random.fold_in(keys[5], 1), TOKENS // TOK_DEV)
    expert_ids_turns = jax.random.permutation(jax.random.fold_in(keys[5], 3), TOKENS // TOK_DEV)
    expert_ids = jax.vmap(lambda own, number: shared_out(jax.random.fold_in(keys[5], 2), own, number, TOK_DEV, EXPERTS, TOP, CAP, 2))(expert_ids_keys, expert_ids_turns).reshape((TOKENS, TOP))
    route_logits = scatter_about(keys[6], (TOKENS, TOP), 1.0, 6.0, ((0, 4),), jnp.float32)
    return {"hidden_states": hidden_states, "norm_gain": norm_gain, "gate_master": gate_master, "up_master": up_master, "down_master": down_master, "expert_ids": expert_ids, "route_logits": route_logits}


EPSILON = 1e-06

def reference(hidden_states, norm_gain, gate_master, up_master, down_master, expert_ids, route_logits):
    scaled = norm_gain[None, :, None]
    gate_serve = (scaled * gate_master).astype(jnp.bfloat16)
    up_serve = (scaled * up_master).astype(jnp.bfloat16)
    down_serve = down_master.astype(jnp.bfloat16)
    values = hidden_states.astype(jnp.float32)
    inv_rms = lax.rsqrt(lax.optimization_barrier(jnp.mean(values * values, axis=1, keepdims=True)) + EPSILON)
    normed = (values * inv_rms).astype(jnp.bfloat16)
    route_weight = jax.nn.softmax(route_logits, axis=1)

    def expert_output(expert):
        gate_pre = jnp.dot(normed, gate_serve[expert], preferred_element_type=jnp.float32)
        up_pre = jnp.dot(normed, up_serve[expert], preferred_element_type=jnp.float32)
        act = (jax.nn.silu(gate_pre) * up_pre).astype(jnp.bfloat16)
        return jnp.dot(act, down_serve[expert].T, preferred_element_type=jnp.float32).astype(jnp.bfloat16)
    outputs = lax.map(expert_output, jnp.arange(EXPERTS, dtype=jnp.int32))
    by_token = jnp.transpose(outputs, (1, 0, 2))
    picked = jnp.take_along_axis(by_token, expert_ids[:, :, None].astype(jnp.int32), axis=1)
    combined = lax.optimization_barrier(jnp.sum(route_weight[:, :, None] * picked.astype(jnp.float32), axis=1)).astype(jnp.bfloat16)
    return (gate_serve, up_serve, down_serve, combined)
```

```python
import functools

import jax
import jax.numpy as jnp
from jax import lax
from jax.experimental import pallas as pl
from jax.experimental.pallas import tpu as pltpu
from jax.sharding import Mesh
from jax.sharding import PartitionSpec as P

AXES = ("z", "y", "c", "x")
EPSILON = 1e-06
BF = jnp.bfloat16
F32 = jnp.float32
H = 224
LANES = 128


def index(z, y, c, x):
    return (((z % 4) * 4 + (y % 4)) * 2 + (c % 2)) * 4 + (x % 4)


def move(value, where):
    pairs = [
        (index(z, y, c, x), index(*where(z, y, c, x)))
        for z in range(4)
        for y in range(4)
        for c in range(2)
        for x in range(4)
    ]
    return lax.ppermute(value, AXES, pairs)


def along_y(value, d):
    return value if d == 0 else move(value, lambda z, y, c, x: (z, y + d, c, x))


def along_z(value, d):
    return value if d == 0 else move(value, lambda z, y, c, x: (z + d, y, c, x))


def along_x(value, d):
    return value if d == 0 else move(value, lambda z, y, c, x: (z, y, c, x + d))


def other_core(value):
    return move(value, lambda z, y, c, x: (z, y, c + 1, x))


def slanted_x(value, k):
    return move(value, lambda z, y, c, x: (z, y, c, x + z + k))


def mirrored_z(value, k):
    return move(value, lambda z, y, c, x: (x - z - k, y, c, x))


SMEM = pl.BlockSpec(memory_space=pltpu.SMEM)
VMEM = pl.BlockSpec(memory_space=pltpu.VMEM)


def call(body, where, inputs, outs, scratch=(), name=None):
    return pl.pallas_call(
        body,
        out_shape=outs,
        in_specs=[SMEM] + [VMEM] * len(inputs),
        out_specs=jax.tree.map(lambda _: VMEM, outs),
        scratch_shapes=list(scratch),
        name=name,
    )(where, *inputs)


def shaped(*shape, dtype=BF):
    return jax.ShapeDtypeStruct(shape, dtype)


def cut(where, gain, weights, by_slant, name):
    scaled = gain is not None

    def body(*refs):
        at = refs[0]
        gain_ref = refs[1] if scaled else None
        w = refs[2] if scaled else refs[1]
        outs = refs[-5:-1]
        turned = refs[-1]
        z, y, c, x = at[0], at[1], at[2], at[3]
        for k in range(4):
            pair = (x + z + k) % 4
            v = w[pl.ds(2 * pair, 2)]
            if scaled:
                v = v * gain_ref[...][None]
            turned[...] = v.astype(BF).reshape(LANES, 8 * H).T
            for dy in range(4):
                for dc in range(2):
                    block = ((y + dy) % 4) * 2 + (c + dc) % 2
                    rows = turned[pl.ds(pl.multiple_of(block * H, 32), H), :]
                    if by_slant:
                        outs[k][dy, dc] = rows
                    else:
                        outs[dy][k, dc] = rows

    inputs = ([gain] if scaled else []) + [weights]
    return call(
        body,
        where,
        inputs,
        [shaped(4, 2, H, LANES)] * 4,
        [pltpu.VMEM((8 * H, LANES), BF)],
        name,
    )


def swap_order(where, pieces, name):
    def body(at, *refs):
        for a in range(4):
            for b in range(4):
                refs[4 + b][a] = refs[a][b]

    return call(body, where, pieces, [shaped(4, 2, H, LANES)] * 4, (), name)


def in_order(where, pieces, by_slant, name):
    def body(at, *refs):
        z, y, c, x = at[0], at[1], at[2], at[3]
        own, send = refs[4], refs[5]
        for a in range(4):
            for b in range(4):
                k, dy = (a, b) if by_slant else (b, a)
                tile = ((x - z - k + 8) % 4) * 4 + (y - dy + 4) % 4
                lane = pl.ds(pl.multiple_of(tile * LANES, LANES), LANES)
                own[:, lane] = refs[a][b, 0]
                send[:, lane] = refs[a][b, 1]

    return call(body, where, pieces, [shaped(H, 16 * LANES)] * 2, (), name)


def halves(a, b):
    first = lax.broadcasted_iota(jnp.int32, a.shape, 1) < 64
    a, b = a.astype(F32), b.astype(F32)
    low = jnp.where(first, a, pltpu.roll(b, 64, 1)).astype(BF)
    high = jnp.where(first, pltpu.roll(a, 64, 1), b).astype(BF)
    return low, high


def settle(where, own, other, name):
    def body(at, own_ref, other_ref, out):
        north = at[2] == 1
        for tile in range(16):
            lane = slice(tile * LANES, (tile + 1) * LANES)
            mine, theirs = own_ref[:, lane], other_ref[:, lane]
            a = jnp.where(north, theirs, mine)
            b = jnp.where(north, mine, theirs)
            low, high = halves(a, b)
            out[0, :, lane] = low
            out[1, :, lane] = high

    return call(body, where, [own, other], shaped(2, H, 16 * LANES), (), name)


def spread(where, mine, theirs):
    def body(at, *refs):
        z, y, c, x = at[0], at[1], at[2], at[3]
        out, scale, total = refs[8], refs[9], refs[10]
        total[...] = jnp.zeros_like(total)
        for which in range(8):
            source = refs[which]
            dz, core = which % 4, (c + which // 4) % 2

            def step(i, _, source=source, dz=dz, core=core):
                dy, dx = i // 4, i % 4
                tile = ((z - dz + 4) % 4) * 4 + (y - dy + 4) % 4
                row = pl.multiple_of(tile * LANES + core * 64, 64)
                lane = pl.ds(pl.multiple_of(((x - dx + 4) % 4) * 512, 512), 512)
                v = source[dy, dx]
                out[pl.ds(row, 64), lane] = v
                f = v.astype(F32)
                total[:, lane] += jnp.sum((f * f).reshape(8, 8, 512), axis=0)
                return 0

            lax.fori_loop(0, 16, step, 0)
        mean = jnp.sum(total[...], axis=0, keepdims=True) / 2048
        scale[...] = lax.rsqrt(mean + EPSILON)

    return call(
        body,
        where,
        list(mine) + list(theirs),
        [shaped(2048, 2048), shaped(1, 2048, dtype=F32)],
        [pltpu.VMEM((8, 2048), F32)],
        "spread",
    )


def activate(gate, up, features, scale, share):
    def body(g_ref, u_ref, x_ref, s_ref, w_ref, out):
        v, s = x_ref[...], s_ref[...]
        for e in range(2):
            g = jnp.dot(g_ref[e], v, preferred_element_type=F32) * s
            u = jnp.dot(u_ref[e], v, preferred_element_type=F32) * s
            act = g / (1.0 + jnp.exp(-g)) * u
            out[e] = (act * w_ref[e : e + 1, :]).astype(BF)

    block = 512
    whole = pl.BlockSpec((2, H, 2048), lambda i: (0, 0, 0))
    return pl.pallas_call(
        body,
        grid=(2048 // block,),
        in_specs=[
            whole,
            whole,
            pl.BlockSpec((2048, block), lambda i: (0, i)),
            pl.BlockSpec((1, block), lambda i: (0, i)),
            pl.BlockSpec((2, block), lambda i: (0, i)),
        ],
        out_specs=pl.BlockSpec((2, H, block), lambda i: (0, 0, i)),
        out_shape=shaped(2, H, 2048),
        name="activate",
    )(gate, up, features, scale, share)


def project(where, own, send, act, act_other):
    def body(at, own_ref, send_ref, a_ref, b_ref, *rest):
        z, y, c, x = at[0], at[1], at[2], at[3]
        ones, twos = rest[:4], rest[4:8]
        down, part = rest[8], rest[9]
        for which, ref in enumerate((own_ref, send_ref)):
            for m in range(8):
                a = ref[:, 2 * m * LANES : (2 * m + 1) * LANES]
                b = ref[:, (2 * m + 1) * LANES : (2 * m + 2) * LANES]
                low, high = halves(a, b)
                lane = slice(m * LANES, (m + 1) * LANES)
                down[(2 * which) * H : (2 * which + 1) * H, lane] = low
                down[(2 * which + 1) * H : (2 * which + 2) * H, lane] = high
        turned = down[...].T
        for i in range(4):
            lane = pl.ds(pl.multiple_of(((x + i) % 4) * 512, 512), 512)
            acts = jnp.concatenate(
                [a_ref[0, :, lane], a_ref[1, :, lane], b_ref[0, :, lane], b_ref[1, :, lane]], axis=0
            )
            got = jnp.dot(turned, acts, preferred_element_type=F32).astype(BF)
            got = got.reshape(4, 4, 64, 512)
            ones[i][...] = got[:, :, :32].reshape(16, 32, 512)
            part[...] = got[:, :, 32:]
            for d in range(4):
                twos[d][:, :, lane] = part[:, (y + d) % 4]

    return call(
        body,
        where,
        [own, send, act, act_other],
        [shaped(16, 32, 512)] * 4 + [shaped(4, 32, 2048)] * 4,
        [pltpu.VMEM((4 * H, 1024), BF), pltpu.VMEM((4, 4, 32, 512), BF)],
        "project",
    )


def add_up(where, pieces, select, outs, name):
    def body(at, *refs):
        coordinates = (at[0], at[1], at[2], at[3])
        for d in range(len(outs)):
            chosen = [select(r, coordinates, d).astype(F32) for r in refs[:4]]
            refs[4 + d][...] = ((chosen[0] + chosen[1]) + (chosen[2] + chosen[3])).astype(BF)

    return call(body, where, pieces, outs, (), name)


def per_device(hidden, gain, gate, up, down, ids, logits):
    where = jnp.stack([lax.axis_index(a) for a in AXES]).astype(jnp.int32)
    x_at = lax.axis_index("x")
    gain = gain.reshape(64, 1)

    share = jax.nn.softmax(logits, axis=1).T
    chosen = ids.T
    experts = jnp.arange(8, dtype=jnp.int32)[:, None]
    table = jnp.where(chosen[0:1] == experts, share[0:1], 0.0) + jnp.where(
        chosen[1:2] == experts, share[1:2], 0.0
    )
    high = table.astype(BF)
    rest = (table - high.astype(F32)).astype(BF)
    tokens = jnp.concatenate([hidden.T, high, rest], axis=0)
    row = [along_x(tokens, d) for d in range(4)]
    line = jnp.stack([r[:64] for r in row])
    table = jnp.stack([r[64:72].astype(F32) + r[72:80].astype(F32) for r in row])
    table = lax.dynamic_slice(table, (0, 2 * x_at, 0), (4, 2, 512))
    table = jnp.stack([lax.dynamic_index_in_dim(table, (x_at - i + 4) % 4, 0, False) for i in range(4)])
    share = jnp.transpose(table, (1, 0, 2)).reshape(2, 2048)
    plane = jnp.stack([along_y(line, d) for d in range(4)])
    mine = [along_z(plane, d) for d in range(4)]
    theirs = [other_core(v) for v in mine]
    features, scale = spread(where, mine, theirs)

    gate_out = cut(where, gain, gate, False, "cut_gate")
    up_out = cut(where, gain, up, True, "cut_up")
    down_out = cut(where, None, down, False, "cut_down")

    def y_x_z(pieces, name):
        pieces = [along_y(p, d) for d, p in enumerate(pieces)]
        pieces = swap_order(where, pieces, "swap_" + name)
        pieces = [slanted_x(p, k) for k, p in enumerate(pieces)]
        pieces = [mirrored_z(p, k) for k, p in enumerate(pieces)]
        return in_order(where, pieces, True, "order_" + name)

    def x_z_y(pieces, name):
        pieces = [slanted_x(p, k) for k, p in enumerate(pieces)]
        pieces = [mirrored_z(p, k) for k, p in enumerate(pieces)]
        pieces = swap_order(where, pieces, "swap_" + name)
        pieces = [along_y(p, d) for d, p in enumerate(pieces)]
        return in_order(where, pieces, False, "order_" + name)

    gate_own, gate_send = y_x_z(gate_out, "gate")
    up_own, up_send = x_z_y(up_out, "up")
    down_own, down_send = y_x_z(down_out, "down")
    gate_serve = settle(where, gate_own, other_core(gate_send), "settle_gate")
    up_serve = settle(where, up_own, other_core(up_send), "settle_up")
    down_serve = settle(where, down_own, other_core(down_send), "settle_down")

    act = activate(gate_serve, up_serve, features, scale, share)
    sums = project(where, down_own, down_send, act, other_core(act))

    one = [along_x(p, d) for d, p in enumerate(sums[:4])]
    one = add_up(
        where, one, lambda r, at, d: r[pl.ds(((at[0] + d) % 4) * 4, 4)], [shaped(4, 32, 512)] * 4, "one_x"
    )
    one = [along_z(p, d) for d, p in enumerate(one)]
    one = add_up(where, one, lambda r, at, d: r[(at[1] + d) % 4], [shaped(32, 512)] * 4, "one_z")
    one = [along_y(p, d) for d, p in enumerate(one)]
    one = add_up(where, one, lambda r, at, d: r[...], [shaped(32, 512)], "one_y")[0]
    two = [along_y(p, d) for d, p in enumerate(sums[4:])]
    two = add_up(where, two, lambda r, at, d: r[(at[0] + d) % 4], [shaped(32, 2048)] * 4, "two_y")
    two = [along_z(p, d) for d, p in enumerate(two)]
    two = add_up(
        where,
        two,
        lambda r, at, d: r[:, pl.ds(pl.multiple_of(((at[3] + d) % 4) * 512, 512), 512)],
        [shaped(32, 512)] * 4,
        "two_z",
    )
    two = [along_x(p, d) for d, p in enumerate(two)]
    two = add_up(where, two, lambda r, at, d: r[...], [shaped(32, 512)], "two_x")[0]
    combined = jnp.concatenate([one, two], axis=0).T
    return tuple(jnp.transpose(w, (0, 2, 1)) for w in (gate_serve, up_serve, down_serve)) + (combined,)


def solution(mesh):
    split = Mesh(mesh.devices.reshape(4, 4, 2, 4), AXES)
    fs = ("z", "y", "c")
    in_specs = (
        P("x", fs),
        P(fs),
        P(None, fs, "x"),
        P(None, fs, "x"),
        P(None, fs, "x"),
        P("x", None),
        P("x", None),
    )
    out_specs = (P("x", None, fs), P("x", None, fs), P("x", None, fs), P("x", fs))
    return jax.shard_map(per_device, mesh=split, in_specs=in_specs, out_specs=out_specs, check_vma=False)
```

```python
import functools

import jax
import jax.numpy as jnp
from jax import lax
from jax.experimental import pallas as pl
from jax.experimental.pallas import tpu as pltpu
from jax.sharding import Mesh
from jax.sharding import PartitionSpec as P

AXES = ("z", "y", "c", "x")
EPSILON = 1e-06
BF = jnp.bfloat16
F32 = jnp.float32
H = 224
LANES = 128


def index(z, y, c, x):
    return (((z % 4) * 4 + (y % 4)) * 2 + (c % 2)) * 4 + (x % 4)


def move(value, where):
    pairs = [
        (index(z, y, c, x), index(*where(z, y, c, x)))
        for z in range(4)
        for y in range(4)
        for c in range(2)
        for x in range(4)
    ]
    return lax.ppermute(value, AXES, pairs)


def along_y(value, d):
    return value if d == 0 else move(value, lambda z, y, c, x: (z, y + d, c, x))


def along_z(value, d):
    return value if d == 0 else move(value, lambda z, y, c, x: (z + d, y, c, x))


def along_x(value, d):
    return value if d == 0 else move(value, lambda z, y, c, x: (z, y, c, x + d))


def other_core(value):
    return move(value, lambda z, y, c, x: (z, y, c + 1, x))


SMEM = pl.BlockSpec(memory_space=pltpu.SMEM)
VMEM = pl.BlockSpec(memory_space=pltpu.VMEM)
MIB = 1 << 20


def shaped(*shape, dtype=BF):
    return pltpu.VMEM(shape, dtype)


def near(values):
    return [pltpu.with_memory_space_constraint(v, pltpu.VMEM) for v in values]


def call(body, where, inputs, outs, scratch=(), name=None, room=8):
    return pl.pallas_call(
        body,
        out_shape=outs,
        in_specs=[SMEM] + [VMEM] * len(inputs),
        out_specs=[VMEM] * len(outs),
        scratch_shapes=list(scratch),
        compiler_params=pltpu.CompilerParams(vmem_limit_bytes=room * MIB),
        name=name,
    )(where, *near(inputs))


def gridded(body, where, inputs, in_specs, outs, out_specs, grid, scratch=(), name=None, room=16):
    return pl.pallas_call(
        body,
        grid=grid,
        in_specs=[SMEM] + in_specs,
        out_specs=out_specs,
        scratch_shapes=list(scratch),
        out_shape=outs,
        compiler_params=pltpu.CompilerParams(vmem_limit_bytes=room * MIB),
        name=name,
    )(where, *inputs)


def cut_by_y(where, gain, weights, name):
    scaled = gain is not None

    def body(*refs):
        at = refs[0]
        w = refs[2] if scaled else refs[1]
        outs, turned = refs[-5:-1], refs[-1]
        v = w[...]
        if scaled:
            v = v * refs[1][...][None]
        turned[...] = v.astype(BF).reshape(LANES, 8 * H).T
        dx = (pl.program_id(0) - at[3] + 4) % 4
        for dy in range(4):
            for dc in range(2):
                block = ((at[1] + dy) % 4) * 2 + (at[2] + dc) % 2
                outs[dy][dx, dc] = turned[pl.ds(pl.multiple_of(block * H, 32), H), :]

    specs = [pl.BlockSpec((2, 64, 8 * H), lambda i: (i, 0, 0))]
    if scaled:
        specs = [pl.BlockSpec((64, 1), lambda i: (0, 0))] + specs
    return gridded(
        body,
        where,
        ([gain] if scaled else []) + [weights],
        specs,
        [shaped(4, 2, H, LANES)] * 4,
        [VMEM] * 4,
        (4,),
        [pltpu.VMEM((8 * H, LANES), BF)],
        name,
    )


def cut_by_x(where, gain, weights, name):
    def body(at, gain_ref, w, *outs):
        half = pl.program_id(0)
        for dx in range(4):
            v = w[pl.ds(2 * ((at[3] + dx) % 4), 2)] * gain_ref[...][None]
            turned = v.astype(BF).reshape(LANES, 4 * H).T
            for j in range(4):
                outs[dx][2 * half + j // 2, j % 2] = turned[j * H : (j + 1) * H]

    return gridded(
        body,
        where,
        [gain, weights],
        [
            pl.BlockSpec((64, 1), lambda i: (0, 0)),
            pl.BlockSpec((8, 64, 4 * H), lambda i: (0, 0, i)),
        ],
        [shaped(4, 2, H, LANES)] * 4,
        [VMEM] * 4,
        (2,),
        (),
        name,
    )


def swap_order(where, pieces, absolute, name):
    def body(at, *refs):
        for a in range(4):
            for b in range(4):
                if absolute:
                    for dc in range(2):
                        refs[4 + b][a, dc] = refs[a][(at[1] + b) % 4, (at[2] + dc) % 2]
                else:
                    refs[4 + b][a] = refs[a][b]

    return call(body, where, pieces, [shaped(4, 2, H, LANES)] * 4, (), name)


def rotate(where, pieces, name):
    def body(at, *refs):
        first = (at[3] - at[0] + 4) % 4
        for turn in range(4):

            @pl.when(first == turn)
            def _(turn=turn):
                def step(i, _):
                    for s in range(4):
                        refs[4 + s][i // 2, i % 2] = refs[(turn - s) % 4][i // 2, i % 2]
                    return 0

                lax.fori_loop(0, 8, step, 0)

    return call(body, where, pieces, [shaped(4, 2, H, LANES)] * 4, (), name)


def halves(a, b):
    first = lax.broadcasted_iota(jnp.int32, a.shape, 1) < 64
    a, b = a.astype(F32), b.astype(F32)
    low = jnp.where(first, a, pltpu.roll(b, 64, 1)).astype(BF)
    high = jnp.where(first, pltpu.roll(a, 64, 1), b).astype(BF)
    return low, high


def settle(where, own, other, by_z, name):
    def body(at, *refs):
        out = refs[8]
        north = at[2] == 1
        rows = pl.ds(pl.multiple_of(pl.program_id(0) * 32, 32), 32)
        for s in range(4):
            for dy in range(4):
                a, b = (s, dy) if by_z else (dy, s)
                mine, theirs = refs[a][b, 0, rows], refs[4 + a][b, 1, rows]
                low, high = halves(jnp.where(north, theirs, mine), jnp.where(north, mine, theirs))
                tile = ((at[0] - s + 4) % 4) * 4 + (at[1] - dy + 4) % 4
                lane = pl.ds(pl.multiple_of(tile * LANES, LANES), LANES)
                out[0, :, lane] = low
                out[1, :, lane] = high

    return gridded(
        body,
        where,
        near(list(own) + list(other)),
        [VMEM] * 8,
        jax.ShapeDtypeStruct((2, H, 16 * LANES), BF),
        pl.BlockSpec((2, 32, 16 * LANES), lambda i: (0, i, 0)),
        (7,),
        (),
        name,
    )


def activate(where, gate, gate_other, up, up_other, mine, theirs, share):
    def body(at, *refs):
        g_refs, g_other, u_refs, u_other = refs[0:4], refs[4:8], refs[8:12], refs[12:16]
        x_refs, x_other, w_ref = refs[16:20], refs[20:24], refs[24]
        out, both, features = refs[25], refs[26], refs[27]

        for s in range(4):
            for dy in range(4):
                lane = slice((s * 4 + dy) * LANES, (s * 4 + dy + 1) * LANES)
                low, high = halves(g_refs[s][dy, 0], g_other[s][dy, 1])
                both[0:H, lane] = low
                both[H : 2 * H, lane] = high
                low, high = halves(u_refs[dy][s, 0], u_other[dy][s, 1])
                both[2 * H : 3 * H, lane] = low
                both[3 * H : 4 * H, lane] = high

        def block(dx, _):
            total = jnp.zeros((8, 512), F32)
            for s in range(4):
                for dy in range(4):
                    for core, source in enumerate((x_refs, x_other)):
                        v = source[s][dy, dx]
                        row = (s * 4 + dy) * LANES + core * 64
                        features[row : row + 64] = v
                        f = v.astype(F32)
                        total = total + jnp.sum((f * f).reshape(8, 8, 512), axis=0)
            scale = lax.rsqrt(jnp.sum(total, axis=0, keepdims=True) / 2048 + EPSILON)
            pre = jnp.dot(both[...], features[...], preferred_element_type=F32) * scale
            for e in range(2):
                g, u = pre[e * H : (e + 1) * H], pre[(2 + e) * H : (3 + e) * H]
                act = g / (1.0 + jnp.exp(-g)) * u
                out[dx, e] = (act * w_ref[dx, e : e + 1, :]).astype(BF)
            return 0

        lax.fori_loop(0, 4, block, 0)

    return call(
        body,
        where,
        [*gate, *gate_other, *up, *up_other, *mine, *theirs, share],
        [shaped(4, 2, H, 512)],
        [pltpu.VMEM((4 * H, 2048), BF), pltpu.VMEM((2048, 512), BF)],
        "activate",
        16,
    )[0]


def project(where, down, act, act_other):
    def body(at, *refs):
        d_refs, a_ref, b_ref = refs[0:4], refs[4], refs[5]
        ones, twos, matrix = refs[6:10], refs[10:14], refs[14]
        for dc in range(2):
            for s in range(4):
                for m in range(2):
                    low, high = halves(d_refs[s][2 * m, dc], d_refs[s][2 * m + 1, dc])
                    lane = slice((s * 2 + m) * LANES, (s * 2 + m + 1) * LANES)
                    matrix[(2 * dc) * H : (2 * dc + 1) * H, lane] = low
                    matrix[(2 * dc + 1) * H : (2 * dc + 2) * H, lane] = high
        turned = matrix[...].T
        for dx in range(4):
            acts = jnp.concatenate([a_ref[dx, 0], a_ref[dx, 1], b_ref[dx, 0], b_ref[dx, 1]], axis=0)
            got = jnp.dot(turned, acts, preferred_element_type=F32).astype(BF)
            got = got.reshape(4, 4, 64, 512)
            ones[dx][...] = got[:, :, :32]
            for dy in range(4):
                twos[dy][:, dx] = got[:, dy, 32:]

    return call(
        body,
        where,
        [*down, act, act_other],
        [shaped(4, 4, 32, 512)] * 8,
        [pltpu.VMEM((4 * H, 1024), BF)],
        "project",
        24,
    )


def add_up(where, pieces, select, outs, name):
    def body(at, *refs):
        for d in range(len(outs)):
            chosen = [select(r, d).astype(F32) for r in refs[:4]]
            refs[4 + d][...] = ((chosen[0] + chosen[1]) + (chosen[2] + chosen[3])).astype(BF)

    return call(body, where, pieces, outs, (), name)


def prepare(where, hidden, ids, logits):
    def body(at, h_ref, i_ref, l_ref, out):
        out[0:64] = h_ref[...]
        first, second = l_ref[0:1], l_ref[1:2]
        top = jnp.maximum(first, second)
        a, b = jnp.exp(first - top), jnp.exp(second - top)
        expert = lax.broadcasted_iota(jnp.int32, (8, 512), 0)
        table = jnp.where(i_ref[0:1] == expert, a / (a + b), 0.0)
        table = table + jnp.where(i_ref[1:2] == expert, b / (a + b), 0.0)
        high = table.astype(BF)
        out[64:80] = jnp.concatenate([high.astype(F32), table - high.astype(F32)], axis=0).astype(BF)

    return call(body, where, [hidden, ids, logits], [shaped(80, 512)], (), "prepare")[0]


def stack_row(where, row):
    def body(at, *refs):
        line, share = refs[4], refs[5]
        expert = lax.broadcasted_iota(jnp.int32, (8, 512), 0)
        for d in range(4):
            line[d] = refs[d][0:64]
            table = refs[d][64:80].astype(F32)
            table = table[0:8] + table[8:16]
            for e in range(2):
                chosen = jnp.where(expert == 2 * at[3] + e, table, 0.0)
                share[d, e : e + 1] = jnp.sum(chosen, axis=0, keepdims=True)

    return call(
        body, where, row, [shaped(4, 64, 512), shaped(4, 2, 512, dtype=F32)], (), "stack_row"
    )


def stack_plane(where, lines):
    def body(at, *refs):
        for d in range(4):
            refs[4][d] = refs[d][...]

    return call(body, where, lines, [shaped(4, 4, 64, 512)], (), "stack_plane")[0]


def finish(where, one, two):
    def body(at, *refs):
        out = refs[8]
        for half in range(2):
            a = [r[...].astype(F32) for r in refs[4 * half : 4 * half + 4]]
            out[32 * half : 32 * half + 32] = ((a[0] + a[1]) + (a[2] + a[3])).astype(BF)

    return call(
        body, where, [*one, *two], [jax.ShapeDtypeStruct((64, 512), BF)], (), "finish"
    )[0]


def per_device(hidden, gain, gate, up, down, ids, logits):
    where = jnp.stack([lax.axis_index(a) for a in AXES]).astype(jnp.int32)
    gain = gain.reshape(64, 1)

    def spread(axis, pieces):
        return [axis(p, d) for d, p in enumerate(pieces)]

    def behind(value, *first):
        return lax.optimization_barrier((value, first))[0]

    tokens = prepare(where, hidden.T, ids.T, logits.T)
    row = [along_x(tokens, d) for d in range(4)]
    up_cut = cut_by_x(behind(where, tokens), gain, up, "cut_up")
    up_pieces = spread(along_x, up_cut)
    gate_cut = cut_by_y(behind(where, up_cut), gain, gate, "cut_gate")
    gate_pieces = spread(along_y, gate_cut)
    line, share = stack_row(behind(where, gate_cut), row)
    plane = [along_y(line, d) for d in range(4)]
    down_cut = cut_by_y(behind(where, line), None, down, "cut_down")
    down_pieces = spread(along_y, down_cut)
    plane = stack_plane(behind(where, down_cut), plane)
    mine = [along_z(plane, d) for d in range(4)]
    up_turned = rotate(behind(where, plane), up_pieces, "rotate_up")
    up_pieces = spread(along_z, up_turned)
    gate_turned = swap_order(behind(where, up_turned), gate_pieces, False, "swap_gate")
    gate_pieces = spread(along_x, gate_turned)
    down_turned = swap_order(behind(where, gate_turned), down_pieces, False, "swap_down")
    down_pieces = spread(along_x, down_turned)
    up_turned = swap_order(behind(where, down_turned), up_pieces, True, "swap_up")
    up_pieces = spread(along_y, up_turned)
    gate_turned = rotate(behind(where, up_turned), gate_pieces, "rotate_gate")
    gate_pieces = spread(along_z, gate_turned)
    down_turned = rotate(behind(where, gate_turned), down_pieces, "rotate_down")
    down_pieces = spread(along_z, down_turned)

    theirs = [other_core(v) for v in mine]
    up_other = [other_core(p) for p in up_pieces]
    gate_other = [other_core(p) for p in gate_pieces]
    down_other = [other_core(p) for p in down_pieces]
    act = activate(
        behind(where, down_turned), gate_pieces, gate_other, up_pieces, up_other, mine, theirs, share
    )
    sums = project(where, down_pieces, act, other_core(act))

    def back(axis, pieces):
        return [axis(p, -d % 4) for d, p in enumerate(pieces)]

    one, two = back(along_x, sums[:4]), back(along_y, sums[4:])
    gate_serve = settle(behind(where, sums), gate_pieces, gate_other, True, "settle_gate")
    one = add_up(behind(where, gate_serve), one, lambda r, d: r[d], [shaped(4, 32, 512)] * 4, "one_x")
    two = add_up(behind(where, one), two, lambda r, d: r[d], [shaped(4, 32, 512)] * 4, "two_y")
    up_serve = settle(behind(where, two), up_pieces, up_other, False, "settle_up")
    one, two = back(along_z, one), back(along_z, two)
    one = add_up(behind(where, up_serve), one, lambda r, d: r[d], [shaped(32, 512)] * 4, "one_z")
    two = add_up(behind(where, one), two, lambda r, d: r[d], [shaped(32, 512)] * 4, "two_z")
    down_serve = settle(behind(where, two), down_pieces, down_other, True, "settle_down")
    one, two = back(along_y, one), back(along_x, two)
    combined = finish(behind(where, down_serve), one, two).T
    return tuple(jnp.transpose(w, (0, 2, 1)) for w in (gate_serve, up_serve, down_serve)) + (combined,)


def solution(mesh):
    split = Mesh(mesh.devices.reshape(4, 4, 2, 4), AXES)
    fs = ("z", "y", "c")
    in_specs = (
        P("x", fs),
        P(fs),
        P(None, fs, "x"),
        P(None, fs, "x"),
        P(None, fs, "x"),
        P("x", None),
        P("x", None),
    )
    out_specs = (P("x", None, fs), P("x", None, fs), P("x", None, fs), P("x", fs))
    return jax.shard_map(per_device, mesh=split, in_specs=in_specs, out_specs=out_specs, check_vma=False)
```
